32 devices in a mesh: fs: 8 (over z, y), tp: 4 (over x, core).
Axes of the slice: x: 2, y: 2, z: 4, core: 2. Of those that a mesh axis runs over, the one named last changes fastest.
Arguments:
- inputs: bfloat16 [48, 4096], P('fs', 'tp'), may hold values from -0.875 to 0.875
- cotangent: bfloat16 [48, 4096], P('fs', 'tp'), may hold values from -8 to 8
- pre_act: bfloat16 [48, 16384], P(None, 'fs'), may hold values from -3 to 3
- w_up: bfloat16 [4096, 16384], P('tp', 'fs'), may hold values from -0.046875 to 0.046875
- w_down: bfloat16 [16384, 4096], P('fs', 'tp'), may hold values from -0.09375 to 0.09375
Outputs:
- grad_input: bfloat16 [48, 4096], P('fs', 'tp')
- grad_up: float32 [4096, 16384], P('tp', 'fs')
- grad_down: float32 [16384, 4096], P('fs', 'tp')
The draws below stay inside these ranges and needn't reach their ends.
All inputs are finite; a program needn't handle non-finite values.
Results may differ from the reference program's by a relative error of at most 0.017.
Values may be sent and summed in bfloat16 or wider, within the bound.
A program may use at most 64 MiB of HBM per device.

```python
import jax
import jax.numpy as jnp

D = 4096
FF = 16384
TOKENS = 48


def spiked(drawn, rng, source, target, blocks, factor):
    def block_of(dim):
        return (jnp.arange(drawn.shape[dim]) // (drawn.shape[dim] // blocks)).reshape((-1,) + (1,) * (drawn.ndim - 1 - dim))

    near = jax.random.permutation(rng, blocks)[block_of(target)]
    second = (block_of(target) + blocks // 2) % blocks
    return jnp.where((block_of(source) == near) | (block_of(source) == second), factor * drawn, drawn)


def shard_levels(rng, extent, pieces, smallest, largest):
    gain, own = 1.0, jax.random.fold_in(rng, 6)
    for axis_at, parts in pieces:
        heights = jnp.exp(jax.random.uniform(jax.random.fold_in(own, axis_at), (parts,), jnp.float32, smallest / len(pieces), largest / len(pieces)))
        gain = gain * jnp.repeat(heights, extent[axis_at] // parts).reshape([-1 if axis == axis_at else 1 for axis in range(len(extent))])
    return gain


def bell_draw(stream_key, shape, deviation, most, shards=(), kind=jnp.bfloat16):
    drawn = deviation * jax.random.normal(stream_key, shape, jnp.float32)
    if shards:
        drawn = drawn * shard_levels(stream_key, shape, shards, -0.22, 0.18)
    return jnp.clip(drawn, -most, most).astype(kind)


def gaussian_with(rng, dims, deviation, bound, cuts, heavy, kind=jnp.bfloat16):
    entries = deviation * jax.random.normal(rng, dims, jnp.float32)
    if cuts:
        entries = entries * shard_levels(rng, dims, cuts, -0.22, 0.18)
    return jnp.clip(spiked(entries, jax.random.fold_in(rng, 3), *heavy), -bound, bound).astype(kind)


def setup_inputs(seed: int = 0) -> dict:
    key_list = jax.random.split(jax.random.key(seed), 6)
    inputs = bell_draw(key_list[0], (TOKENS, D), (TOKENS ** -0.5), 0.875, ((0, 8), (1, 4)))
    cotangent = gaussian_with(key_list[1], (TOKENS, D), 1.0, 8.0, ((0, 8), (1, 4)), (0, 1, 8, 2.0))
    pre_act = gaussian_with(key_list[2], (TOKENS, FF), (TOKENS ** -0.25), 3.0, ((1, 8),), (1, 0, 8, 2.0))
    w_up = bell_draw(key_list[3], (D, FF), FF ** -0.5, 0.046875, ((0, 4), (1, 8)))
    w_down = bell_draw(key_list[4], (FF, D), D ** -0.5, 0.09375, ((0, 8), (1, 4)))
    return {"inputs": inputs, "cotangent": cotangent, "pre_act": pre_act, "w_up": w_up, "w_down": w_down}


def reference(inputs, cotangent, pre_act, w_up, w_down):
    active = jax.nn.relu(pre_act.astype(jnp.float32))
    act = jnp.square(active).astype(jnp.bfloat16)
    hidden = jnp.dot(cotangent, w_down.T, preferred_element_type=jnp.float32)
    grad_pre = (2.0 * active * hidden).astype(jnp.bfloat16)
    grad_down = jnp.dot(act.T, cotangent, preferred_element_type=jnp.float32)
    grad_up = jnp.dot(inputs.T, grad_pre, preferred_element_type=jnp.float32)
    grad_input = jnp.dot(grad_pre, w_up.T, preferred_element_type=jnp.float32).astype(jnp.bfloat16)
    return grad_input, grad_up, grad_down
```

```python
import functools

import jax
import jax.numpy as jnp
from jax import lax
from jax.experimental import pallas as pl
from jax.experimental.pallas import tpu as pltpu
from jax.sharding import PartitionSpec as P

F32, BF16 = jnp.float32, jnp.bfloat16
SLAB = 8
NT = (((1,), (1,)), ((), ()))
TN = (((0,), (0,)), ((), ()))
NN = (((1,), (0,)), ((), ()))


def dot(a, b, dims):
    return lax.dot_general(a, b, dims, preferred_element_type=F32)


def exchange(
    n,
    chips,
    chunks,
    cot_ref,
    in_ref,
    pre_ref,
    wu_ref,
    wd_ref,
    cot_out,
    in_out,
    act_out,
    gp_out,
    gi_out,
    cot_v,
    in_v,
    pre_v,
    wu_v,
    wd_v,
    cot_g,
    in_g,
    spread,
    cot_2,
    cot_f,
    active_f,
    gp_f,
    own,
    p1_s,
    p1_r,
    p2_s,
    p2_r,
    gp_2,
    rs_s,
    rs_r,
    local,
    cs,
    cr,
    is_,
    ir,
    s1,
    r1,
    s2,
    r2,
    s3,
    r3,
    s4,
    r4,
):
    me = lax.axis_index("fs")
    tp = lax.axis_index("tp")
    core = lax.rem(tp, 2)
    rows = cot_v.shape[0]
    width = wd_v.shape[1]
    half = n // 2
    group = half * rows
    side, place_in = me // half, lax.rem(me, half)
    sides = (side, 1 - side)
    first_row = [pl.multiple_of(g * group, 8) for g in sides]
    near = [half * side + lax.rem(place_in + k, half) for k in range(1, half)]
    far = [half * (1 - side) + q for q in range(half)]
    partner = tp + 1 - 2 * core
    x_peer = [None] + [lax.rem(tp + 2 * k, 2 * chips) for k in range(1, chips)]

    barrier = pltpu.get_barrier_semaphore()
    for p in far + near:
        pl.semaphore_signal(barrier, inc=1, device_id={"fs": p})
    pl.semaphore_signal(barrier, inc=1, device_id={"tp": partner})

    @pl.when(core == 1)
    def _():
        for k in range(1, chips):
            pl.semaphore_signal(barrier, inc=1, device_id={"tp": x_peer[k]})

    load_cot = pltpu.make_async_copy(cot_ref, cot_v, local.at[0])
    load_in = pltpu.make_async_copy(in_ref, in_v, local.at[1])
    load_cot.start()
    load_in.start()
    load_wd, load_pre, load_wu = [], [], []
    for j in range(chunks):
        load_wd.append(
            pltpu.make_async_copy(
                wd_ref.at[pl.ds(j * width, width)], wd_v.at[j], local.at[4 + j]
            )
        )
        load_wd[-1].start()
    for j in range(chunks):
        load_pre.append(
            pltpu.make_async_copy(
                pre_ref.at[:, pl.ds(j * width, width)],
                pre_v.at[j],
                local.at[4 + chunks + j],
            )
        )
        load_pre[-1].start()
    for j in range(chunks):
        load_wu.append(
            pltpu.make_async_copy(
                wu_ref.at[:, pl.ds(j * width, width)],
                wu_v.at[j],
                local.at[4 + 2 * chunks + j],
            )
        )
        load_wu[-1].start()
    spread[...] = jnp.zeros_like(spread)
    load_cot.wait()
    load_in.wait()
    own_cot = pltpu.make_async_copy(cot_v, cot_g.at[me], local.at[2])
    own_in = pltpu.make_async_copy(in_v, in_g.at[me], local.at[3])
    own_cot.start()
    own_in.start()

    def to_fs(src, dst, send_sem, recv_sem, p):
        return pltpu.make_async_remote_copy(
            src, dst.at[me], send_sem.at[p], recv_sem.at[me], device_id={"fs": p}
        )

    def from_fs(src, dst, send_sem, recv_sem, p):
        return pltpu.make_async_remote_copy(
            src, dst.at[p], send_sem.at[p], recv_sem.at[p], device_id={"fs": p}
        )

    pl.semaphore_wait(barrier, n + core * (chips - 1))
    for p in far[::-1] + near:
        to_fs(cot_v, cot_g, cs, cr, p).start()

    def picker(shape, token_dim):
        t = lax.broadcasted_iota(jnp.int32, shape, token_dim)
        j = lax.broadcasted_iota(jnp.int32, shape, 1 - token_dim)
        q, r = j // SLAB, j % SLAB
        return ((t == q * rows + r) & (r < rows)).astype(F32).astype(BF16)

    pick = picker((group, half * SLAB), 0)
    place = picker((half * SLAB, group), 1)

    def gathered(ref, g):
        for s in range(half):
            spread[s * SLAB : s * SLAB + rows, :] = ref[half * g + s].astype(F32)
        return dot(pick, spread[...].astype(BF16), NN)

    def gather_cot(ph):
        for p in (near, far)[ph]:
            from_fs(cot_v, cot_g, cs, cr, p).wait_recv()
        block = gathered(cot_g, sides[ph])
        cot_f[pl.ds(first_row[ph], group), :] = block
        cot_2[ph] = block.astype(BF16)

    def between(src, dst, send_sem, recv_sem, ph, j, to):
        return pltpu.make_async_remote_copy(
            src.at[ph, j],
            dst.at[ph, j],
            send_sem.at[ph, j],
            recv_sem.at[ph, j],
            device_id={"tp": to},
        )

    def to_chip(ph, j, k):
        return pltpu.make_async_remote_copy(
            p2_s.at[ph, j],
            p2_r.at[k - 1, ph, j],
            s2.at[k - 1, ph, j],
            r2.at[k - 1, ph, j],
            device_id={"tp": x_peer[k]},
        )

    def first_sum(ph, j):
        return between(p1_s, p1_r, s1, r1, ph, j, partner)

    def share(ph, j):
        return between(gp_2, gp_2, s3, r3, ph, j, partner)

    def lower(ph):
        for j in range(chunks):
            p1_s[ph, j] = dot(cot_2[ph], wd_v[j], NT).astype(BF16)
            first_sum(ph, j).start()

    def join(ph, j):
        first_sum(ph, j).wait_recv()
        total = own[ph, j] + p1_r[ph, j].astype(F32)
        own[ph, j] = total
        p2_s[ph, j] = total.astype(BF16)
        for k in range(1, chips):
            to_chip(ph, j, k).start()

    def upper(ph):
        own[ph, 0] = dot(cot_2[ph], wd_v[0], NT)
        for j in range(1, chunks):
            own[ph, j] = dot(cot_2[ph], wd_v[j], NT)
            join(ph, j - 1)
        join(ph, chunks - 1)

    def keep(ph, j):
        gp_f[j, pl.ds(first_row[ph], group), :] = gp_2[ph, j].astype(F32)

    def finish(ph, j):
        hidden = own[ph, j]
        for k in range(1, chips):
            to_chip(ph, j, k).wait_recv()
            hidden = hidden + p2_r[k - 1, ph, j].astype(F32)
        active = active_f[j, pl.ds(first_row[ph], group), :]
        gp_2[ph, j] = (2.0 * active * hidden).astype(BF16)
        share(ph, j).start()

    def accumulate_lower(ph):
        acc = None
        for j in range(chunks):
            share(ph, j).wait_recv()
            term = dot(gp_2[ph, j], wu_v[j], NT)
            acc = term if acc is None else acc + term
        return acc

    def accumulate_upper(ph):
        acc = None
        for j in range(chunks):
            finish(ph, j)
            term = dot(gp_2[ph, j], wu_v[j], NT)
            acc = term if acc is None else acc + term
        return acc

    def scatter_copies(ph):
        if ph == 0:
            return [
                pltpu.make_async_remote_copy(
                    rs_s.at[0, lax.rem(place_in + k, half)],
                    rs_r.at[k],
                    s4.at[k],
                    r4.at[k],
                    device_id={"fs": near[k - 1]},
                )
                for k in range(1, half)
            ]
        return [
            pltpu.make_async_remote_copy(
                rs_s.at[1, q],
                rs_r.at[half + place_in],
                s4.at[half + q],
                r4.at[half + place_in],
                device_id={"fs": far[q]},
            )
            for q in range(half)
        ]

    def scatter(ph, acc):
        slabs = dot(place, acc.astype(BF16), NN)
        for s in range(half):
            rs_s[ph, s] = slabs[s * SLAB : s * SLAB + rows, :].astype(BF16)
        for copy in scatter_copies(ph):
            copy.start()

    def share_inputs():
        for p in far + near:
            to_fs(in_v, in_g, is_, ir, p).start()

    def activate():
        for copy in load_pre:
            copy.wait()
        for j in range(chunks):
            active = jnp.maximum(pre_v[j].astype(F32), 0.0)
            active_f[j] = active
            act_out[j] = (active * active).astype(BF16)

    for copy in load_wd:
        copy.wait()
    own_cot.wait()
    gather_cot(0)

    @pl.when(core == 0)
    def _():
        lower(0)
        gather_cot(1)
        lower(1)
        share_inputs()
        activate()
        for copy in load_wu:
            copy.wait()
        scatter(0, accumulate_lower(0))
        scatter(1, accumulate_lower(1))

    @pl.when(core == 1)
    def _():
        upper(0)
        gather_cot(1)
        upper(1)
        share_inputs()
        activate()
        for copy in load_wu:
            copy.wait()
        scatter(0, accumulate_upper(0))
        scatter(1, accumulate_upper(1))

    cot_out[...] = cot_f[...].astype(BF16)
    for ph in range(2):
        for j in range(chunks):
            keep(ph, j)
    gp_out[...] = gp_f[...].astype(BF16)
    own_in.wait()
    for p in near + far:
        from_fs(in_v, in_g, is_, ir, p).wait_recv()
    for g in range(2):
        cot_f[g * group : (g + 1) * group, :] = gathered(in_g, g)
    in_out[...] = cot_f[...].astype(BF16)

    for p in far + near:
        to_fs(cot_v, cot_g, cs, cr, p).wait_send()
        to_fs(in_v, in_g, is_, ir, p).wait_send()

    @pl.when(core == 0)
    def _():
        for ph in range(2):
            for j in range(chunks):
                first_sum(ph, j).wait_send()

    @pl.when(core == 1)
    def _():
        for ph in range(2):
            for j in range(chunks):
                for k in range(1, chips):
                    to_chip(ph, j, k).wait_send()
                share(ph, j).wait_send()

    total = rs_s[0, place_in].astype(F32)
    for copy, k in zip(scatter_copies(0), range(1, half)):
        copy.wait_recv()
        total = total + rs_r[k].astype(F32)
    for q in range(half):
        pltpu.make_async_remote_copy(
            rs_s.at[1, q],
            rs_r.at[half + q],
            s4.at[half + q],
            r4.at[half + q],
            device_id={"fs": far[q]},
        ).wait_recv()
        total = total + rs_r[half + q].astype(F32)
    gi_out[...] = total.astype(BF16)
    for ph in range(2):
        for copy in scatter_copies(ph):
            copy.wait_send()


def outer(
    chunks, cot_v, in_v, act_v, gp_v, gi_v, gi_out, gu_out, gd_out, gu_v, gd_v, sem
):
    width = gp_v.shape[2]
    pieces = []

    def put(src, dst):
        copy = pltpu.make_async_copy(src, dst, sem.at[len(pieces)])
        copy.start()
        pieces.append(copy)

    half = width // 2
    for j in range(chunks):
        for h in range(2):
            rows = pl.ds(j * width + h * half, half)
            gd_v[rows, :] = dot(act_v[j, :, h * half : (h + 1) * half], cot_v[...], TN)
            put(gd_v.at[rows], gd_out.at[rows])
    put(gi_v, gi_out)
    step = in_v.shape[1] // (2 * chunks)
    for i in range(2 * chunks):
        rows = pl.ds(i * step, step)
        for j in range(chunks):
            gu_v[rows, j * width : (j + 1) * width] = dot(
                in_v[:, i * step : (i + 1) * step], gp_v[j], TN
            )
        put(gu_v.at[rows], gu_out.at[rows])
    for copy in pieces:
        copy.wait()


def fused(n, ntp, inputs, cotangent, pre_act, w_up, w_down):
    rows, d = inputs.shape
    tokens, ff = pre_act.shape
    chips = ntp // 2
    half = n // 2
    group = half * rows
    chunks = 4 if ff % 1024 == 0 else 2
    width = ff // chunks
    hbm = pl.BlockSpec(memory_space=pl.ANY)
    vmem = pl.BlockSpec(memory_space=pltpu.VMEM)
    dma = pltpu.SemaphoreType.DMA
    cot, full, act, gp, gi = pl.pallas_call(
        functools.partial(exchange, n, chips, chunks),
        out_shape=(
            pltpu.VMEM((tokens, d), BF16),
            pltpu.VMEM((tokens, d), BF16),
            pltpu.VMEM((chunks, tokens, width), BF16),
            pltpu.VMEM((chunks, tokens, width), BF16),
            pltpu.VMEM((rows, d), BF16),
        ),
        in_specs=[hbm] * 5,
        out_specs=(vmem,) * 5,
        scratch_shapes=[
            pltpu.VMEM((rows, d), BF16),
            pltpu.VMEM((rows, d), BF16),
            pltpu.VMEM((chunks, tokens, width), BF16),
            pltpu.VMEM((chunks, d, width), BF16),
            pltpu.VMEM((chunks, width, d), BF16),
            pltpu.VMEM((n, rows, d), BF16),
            pltpu.VMEM((n, rows, d), BF16),
            pltpu.VMEM((half * SLAB, d), F32),
            pltpu.VMEM((2, group, d), BF16),
            pltpu.VMEM((tokens, d), F32),
            pltpu.VMEM((chunks, tokens, width), F32),
            pltpu.VMEM((chunks, tokens, width), F32),
            pltpu.VMEM((2, chunks, group, width), F32),
            pltpu.VMEM((2, chunks, group, width), BF16),
            pltpu.VMEM((2, chunks, group, width), BF16),
            pltpu.VMEM((2, chunks, group, width), BF16),
            pltpu.VMEM((chips - 1, 2, chunks, group, width), BF16),
            pltpu.VMEM((2, chunks, group, width), BF16),
            pltpu.VMEM((2, half, rows, d), BF16),
            pltpu.VMEM((n, rows, d), BF16),
            dma((4 + 3 * chunks,)),
            dma((n,)),
            dma((n,)),
            dma((n,)),
            dma((n,)),
            dma((2, chunks)),
            dma((2, chunks)),
            dma((chips - 1, 2, chunks)),
            dma((chips - 1, 2, chunks)),
            dma((2, chunks)),
            dma((2, chunks)),
            dma((n,)),
            dma((n,)),
        ],
        compiler_params=pltpu.CompilerParams(collective_id=0, has_side_effects=True),
    )(cotangent, inputs, pre_act, w_up, w_down)
    return pl.pallas_call(
        functools.partial(outer, chunks),
        out_shape=(
            jax.ShapeDtypeStruct((rows, d), BF16),
            jax.ShapeDtypeStruct((d, ff), F32),
            jax.ShapeDtypeStruct((ff, d), F32),
        ),
        in_specs=[vmem] * 5,
        out_specs=(hbm,) * 3,
        scratch_shapes=[
            pltpu.VMEM((d, ff), F32),
            pltpu.VMEM((ff, d), F32),
            dma((4 * chunks + 1,)),
        ],
    )(*(pltpu.with_memory_space_constraint(x, pltpu.VMEM) for x in (cot, full, act, gp, gi)))


def plain(inputs, cotangent, pre_act, w_up, w_down):
    active = jax.nn.relu(pre_act.astype(F32))
    squared = jnp.square(active).astype(BF16)
    piece = lax.all_gather(cotangent, "fs", axis=0, tiled=True)
    grad_down = dot(squared, piece, TN)
    hidden = lax.psum(dot(piece, w_down, NT).astype(BF16), "tp").astype(F32)
    grad_pre = (2.0 * active * hidden).astype(BF16)
    grad_up = dot(lax.all_gather(inputs, "fs", axis=0, tiled=True), grad_pre, TN)
    grad_input = lax.psum_scatter(
        dot(grad_pre, w_up, NT), "fs", scatter_dimension=0, tiled=True
    ).astype(BF16)
    return (grad_input, grad_up, grad_down)


def solution(mesh):
    n, ntp = mesh.shape["fs"], mesh.shape["tp"]

    def body(inputs, cotangent, pre_act, w_up, w_down):
        rows, d = inputs.shape
        tokens, ff = pre_act.shape
        if (
            n == 8
            and ntp > 2
            and ntp % 2 == 0
            and rows <= SLAB
            and tokens % 16 == 0
            and d % 1024 == 0
            and ff % 1024 == 0
        ):
            return fused(n, ntp, inputs, cotangent, pre_act, w_up, w_down)
        return plain(inputs, cotangent, pre_act, w_up, w_down)

    return jax.shard_map(
        body,
        mesh=mesh,
        in_specs=(P("fs", "tp"), P("fs", "tp"), P(None, "fs"), P("tp", "fs"), P("fs", "tp")),
        out_specs=(P("fs", "tp"), P("tp", "fs"), P("fs", "tp")),
        check_vma=False,
    )
```

```python
import functools

import jax
import jax.numpy as jnp
from jax import lax
from jax.experimental import pallas as pl
from jax.experimental.pallas import tpu as pltpu
from jax.sharding import PartitionSpec as P

F32, BF16 = jnp.float32, jnp.bfloat16
SLAB = 8
CHUNKS = 4
RAW = 4
NT = (((1,), (1,)), ((), ()))
TN = (((0,), (0,)), ((), ()))
NN = (((1,), (0,)), ((), ()))


def dot(a, b, dims):
    return lax.dot_general(a, b, dims, preferred_element_type=F32)


def exchange(
    n,
    chips,
    chunks,
    direct,
    cot_ref,
    in_ref,
    pre_ref,
    wu_ref,
    wd_ref,
    cot_out,
    in_out,
    act_out,
    gp_out,
    gi_out,
    cot_v,
    in_v,
    pre_v,
    wu_v,
    wd_v,
    cot_g,
    in_g,
    spread,
    own,
    p1_s,
    p1_r,
    p2_s,
    p2_r,
    raw_r,
    rs_s,
    rs_r,
    local,
    cs,
    cr,
    is_,
    ir,
    s1,
    r1,
    s2,
    r2,
    s3,
    r3,
    s4,
    r4,
    s5,
    r5,
    ready,
):
    me = lax.axis_index("fs")
    tp = lax.axis_index("tp")
    core = lax.rem(tp, 2)
    rows = cot_v.shape[0]
    width = wd_v.shape[1]
    tokens = n * rows
    half = n // 2
    side, spot = me // half, lax.rem(me, half)
    near = [half * side + lax.rem(spot + k, half) for k in range(1, half)]
    far = [half * (1 - side) + q for q in range(half)]
    partner = tp + 1 - 2 * core
    x_peer = [None] + [lax.rem(tp + 1 - core + 2 * k, 2 * chips) for k in range(1, chips)]

    barrier = pltpu.get_barrier_semaphore()
    for p in far + near:
        pl.semaphore_signal(barrier, inc=1, device_id={"fs": p})
    pl.semaphore_signal(barrier, inc=1, device_id={"tp": partner})

    @pl.when(core == 1)
    def _():
        for k in range(1, chips):
            pl.semaphore_signal(barrier, inc=1, device_id={"tp": x_peer[k]})

    load_cot = pltpu.make_async_copy(cot_ref, cot_v, local.at[0])
    load_in = pltpu.make_async_copy(in_ref, in_v, local.at[1])
    load_cot.start()
    load_in.start()
    load_wd, load_pre, load_wu = [], [], []
    for j in range(chunks):
        load_wd.append(
            pltpu.make_async_copy(
                wd_ref.at[pl.ds(j * width, width)], wd_v.at[j], local.at[4 + j]
            )
        )
        load_wd[-1].start()
    for j in range(chunks):
        load_pre.append(
            pltpu.make_async_copy(
                pre_ref.at[:, pl.ds(j * width, width)],
                pre_v.at[j],
                local.at[4 + chunks + j],
            )
        )
        load_pre[-1].start()
    for j in range(chunks):
        load_wu.append(
            pltpu.make_async_copy(
                wu_ref.at[:, pl.ds(j * width, width)],
                wu_v.at[j],
                local.at[4 + 2 * chunks + j],
            )
        )
        load_wu[-1].start()
    spread[...] = jnp.zeros_like(spread)
    load_cot.wait()
    load_in.wait()
    own_cot = pltpu.make_async_copy(cot_v, cot_g.at[me], local.at[2])
    own_in = pltpu.make_async_copy(in_v, in_g.at[me], local.at[3])
    own_cot.start()
    own_in.start()

    def to_fs(src, dst, send_sem, recv_sem, p):
        return pltpu.make_async_remote_copy(
            src, dst.at[me], send_sem.at[p], recv_sem.at[me], device_id={"fs": p}
        )

    def from_fs(src, dst, send_sem, recv_sem, p):
        return pltpu.make_async_remote_copy(
            src, dst.at[p], send_sem.at[p], recv_sem.at[p], device_id={"fs": p}
        )

    pl.semaphore_wait(barrier, n + core * (chips - 1))

    @pl.when(core == 1)
    def _():
        pl.semaphore_signal(ready, inc=1, device_id={"tp": partner})

    for p in far[::-1] + near:
        to_fs(cot_v, cot_g, cs, cr, p).start()

    def picker(shape, token_dim):
        t = lax.broadcasted_iota(jnp.int32, shape, token_dim)
        j = lax.broadcasted_iota(jnp.int32, shape, 1 - token_dim)
        q, r = j // SLAB, j % SLAB
        return ((t == q * rows + r) & (r < rows)).astype(F32).astype(BF16)

    pick = picker((tokens, n * SLAB), 0)
    place = picker((n * SLAB, tokens), 1)

    def gathered(ref):
        for s in range(n):
            spread[s * SLAB : s * SLAB + rows, :] = ref[s].astype(F32)
        return spread[...].astype(BF16)

    def between(src, dst, send_sem, recv_sem, j):
        return pltpu.make_async_remote_copy(
            src.at[j], dst.at[j], send_sem.at[j], recv_sem.at[j], device_id={"tp": partner}
        )

    def to_chip(j, k):
        return pltpu.make_async_remote_copy(
            p2_s.at[j],
            p2_r.at[k - 1, j],
            s2.at[k - 1, j],
            r2.at[k - 1, j],
            device_id={"tp": x_peer[k]},
        )

    def direct_to_chip(j, k, src, c):
        return pltpu.make_async_remote_copy(
            src.at[j],
            raw_r.at[k - 1, c, j],
            s5.at[k - 1, j],
            r5.at[k - 1, c, j],
            device_id={"tp": x_peer[k]},
        )

    def first_sum(j):
        return between(p1_s, p1_r, s1, r1, j)

    def share(j):
        return between(gp_out, gp_out, s3, r3, j)

    def lower():
        for j in range(chunks):
            p1_s[j] = dot(cot_out[...], wd_v[j], NT).astype(BF16)
            first_sum(j).start()
            if j == 0:
                pl.semaphore_wait(ready, 1)
            if j < direct:
                for k in range(1, chips):
                    direct_to_chip(j, k, p1_s, 0).start()

    def join(j):
        first_sum(j).wait_recv()
        total = own[j] + p1_r[j].astype(F32)
        own[j] = total
        p2_s[j] = total.astype(BF16)
        for k in range(1, chips):
            to_chip(j, k).start()

    def upper():
        for j in range(chunks):
            own[j] = dot(cot_out[...], wd_v[j], NT)
            if j < direct:
                p2_s[j] = own[j].astype(BF16)
                for k in range(1, chips):
                    direct_to_chip(j, k, p2_s, 1).start()
        for j in range(direct, chunks):
            join(j)

    def finish(j):
        hidden = own[j]
        if j < direct:
            first_sum(j).wait_recv()
            hidden = hidden + p1_r[j].astype(F32)
        for k in range(1, chips):
            if j < direct:
                for c in (1, 0):
                    direct_to_chip(j, k, p2_s, c).wait_recv()
                    hidden = hidden + raw_r[k - 1, c, j].astype(F32)
            else:
                to_chip(j, k).wait_recv()
                hidden = hidden + p2_r[k - 1, j].astype(F32)
        active = jnp.maximum(pre_v[j].astype(F32), 0.0)
        gp = (2.0 * active * hidden).astype(BF16)
        gp_out[j] = dot(place, gp, NN).astype(BF16)
        share(j).start()

    def obtain(j):
        share(j).wait_recv()

    def accumulate(ready):
        acc = None
        for j in range(chunks):
            ready(j)
            term = dot(gp_out[j], wu_v[j], NT)
            acc = term if acc is None else acc + term
        for s in range(n):
            rs_s[s] = acc[s * SLAB : s * SLAB + rows, :].astype(BF16)
        for p in far + near:
            to_fs(rs_s.at[p], rs_r, s4, r4, p).start()

    def share_inputs():
        for p in far + near:
            to_fs(in_v, in_g, is_, ir, p).start()

    def activate():
        for copy in load_pre:
            copy.wait()
        for j in range(chunks):
            active = jnp.maximum(pre_v[j].astype(F32), 0.0)
            act_out[j] = (active * active).astype(BF16)

    for copy in load_wd:
        copy.wait()
    own_cot.wait()
    for p in near + far:
        from_fs(cot_v, cot_g, cs, cr, p).wait_recv()
    cot_out[...] = dot(pick, gathered(cot_g), NN).astype(BF16)

    @pl.when(core == 0)
    def _():
        lower()
        share_inputs()
        activate()
        for copy in load_wu:
            copy.wait()
        accumulate(obtain)

    @pl.when(core == 1)
    def _():
        upper()
        share_inputs()
        activate()
        for copy in load_wu:
            copy.wait()
        accumulate(finish)

    own_in.wait()
    for p in near + far:
        from_fs(in_v, in_g, is_, ir, p).wait_recv()
    in_out[...] = gathered(in_g)

    for p in far + near:
        to_fs(cot_v, cot_g, cs, cr, p).wait_send()
        to_fs(in_v, in_g, is_, ir, p).wait_send()

    @pl.when(core == 0)
    def _():
        for j in range(chunks):
            first_sum(j).wait_send()
            if j < direct:
                for k in range(1, chips):
                    direct_to_chip(j, k, p1_s, 0).wait_send()

    @pl.when(core == 1)
    def _():
        for j in range(chunks):
            for k in range(1, chips):
                if j < direct:
                    direct_to_chip(j, k, p2_s, 1).wait_send()
                else:
                    to_chip(j, k).wait_send()
            share(j).wait_send()

    total = rs_s[me].astype(F32)
    for p in near + far:
        from_fs(rs_s.at[p], rs_r, s4, r4, p).wait_recv()
        total = total + rs_r[p].astype(F32)
    gi_out[...] = total.astype(BF16)
    for p in far + near:
        to_fs(rs_s.at[p], rs_r, s4, r4, p).wait_send()


def outer(
    chunks, cot_v, in_v, act_v, gp_v, gi_v, gi_out, gu_out, gd_out, gu_v, gd_v, sem
):
    width = gp_v.shape[2]
    pieces = []

    def put(src, dst):
        copy = pltpu.make_async_copy(src, dst, sem.at[len(pieces)])
        copy.start()
        pieces.append(copy)

    half = width // 2
    for j in range(chunks):
        for h in range(2):
            rows = pl.ds(j * width + h * half, half)
            gd_v[rows, :] = dot(act_v[j, :, h * half : (h + 1) * half], cot_v[...], TN)
            put(gd_v.at[rows], gd_out.at[rows])
    put(gi_v, gi_out)
    step = in_v.shape[1] // (2 * chunks)
    for i in range(2 * chunks):
        rows = pl.ds(i * step, step)
        for j in range(chunks):
            gu_v[rows, j * width : (j + 1) * width] = dot(
                in_v[:, i * step : (i + 1) * step], gp_v[j], TN
            )
        put(gu_v.at[rows], gu_out.at[rows])
    for copy in pieces:
        copy.wait()


def fused(n, ntp, inputs, cotangent, pre_act, w_up, w_down):
    rows, d = inputs.shape
    tokens, ff = pre_act.shape
    chips = ntp // 2
    chunks = CHUNKS
    width = ff // chunks
    hbm = pl.BlockSpec(memory_space=pl.ANY)
    vmem = pl.BlockSpec(memory_space=pltpu.VMEM)
    dma = pltpu.SemaphoreType.DMA
    cot, full, act, gp, gi = pl.pallas_call(
        functools.partial(exchange, n, chips, chunks, RAW),
        out_shape=(
            pltpu.VMEM((tokens, d), BF16),
            pltpu.VMEM((n * SLAB, d), BF16),
            pltpu.VMEM((chunks, tokens, width), BF16),
            pltpu.VMEM((chunks, n * SLAB, width), BF16),
            pltpu.VMEM((rows, d), BF16),
        ),
        in_specs=[hbm] * 5,
        out_specs=(vmem,) * 5,
        scratch_shapes=[
            pltpu.VMEM((rows, d), BF16),
            pltpu.VMEM((rows, d), BF16),
            pltpu.VMEM((chunks, tokens, width), BF16),
            pltpu.VMEM((chunks, d, width), BF16),
            pltpu.VMEM((chunks, width, d), BF16),
            pltpu.VMEM((n, rows, d), BF16),
            pltpu.VMEM((n, rows, d), BF16),
            pltpu.VMEM((n * SLAB, d), F32),
            pltpu.VMEM((chunks, tokens, width), F32),
            pltpu.VMEM((chunks, tokens, width), BF16),
            pltpu.VMEM((chunks, tokens, width), BF16),
            pltpu.VMEM((chunks, tokens, width), BF16),
            pltpu.VMEM((chips - 1, chunks, tokens, width), BF16),
            pltpu.VMEM((chips - 1, 2, RAW, tokens, width), BF16),
            pltpu.VMEM((n, rows, d), BF16),
            pltpu.VMEM((n, rows, d), BF16),
            dma((4 + 3 * chunks,)),
            dma((n,)),
            dma((n,)),
            dma((n,)),
            dma((n,)),
            dma((chunks,)),
            dma((chunks,)),
            dma((chips - 1, chunks)),
            dma((chips - 1, chunks)),
            dma((chunks,)),
            dma((chunks,)),
            dma((n,)),
            dma((n,)),
            dma((chips - 1, RAW)),
            dma((chips - 1, 2, RAW)),
            pltpu.SemaphoreType.REGULAR,
        ],
        compiler_params=pltpu.CompilerParams(collective_id=0, has_side_effects=True),
    )(cotangent, inputs, pre_act, w_up, w_down)
    return pl.pallas_call(
        functools.partial(outer, chunks),
        out_shape=(
            jax.ShapeDtypeStruct((rows, d), BF16),
            jax.ShapeDtypeStruct((d, ff), F32),
            jax.ShapeDtypeStruct((ff, d), F32),
        ),
        in_specs=[vmem] * 5,
        out_specs=(hbm,) * 3,
        scratch_shapes=[
            pltpu.VMEM((d, ff), F32),
            pltpu.VMEM((ff, d), F32),
            dma((4 * chunks + 1,)),
        ],
    )(*(pltpu.with_memory_space_constraint(x, pltpu.VMEM) for x in (cot, full, act, gp, gi)))


def plain(inputs, cotangent, pre_act, w_up, w_down):
    active = jax.nn.relu(pre_act.astype(F32))
    squared = jnp.square(active).astype(BF16)
    piece = lax.all_gather(cotangent, "fs", axis=0, tiled=True)
    grad_down = dot(squared, piece, TN)
    hidden = lax.psum(dot(piece, w_down, NT).astype(BF16), "tp").astype(F32)
    grad_pre = (2.0 * active * hidden).astype(BF16)
    grad_up = dot(lax.all_gather(inputs, "fs", axis=0, tiled=True), grad_pre, TN)
    grad_input = lax.psum_scatter(
        dot(grad_pre, w_up, NT), "fs", scatter_dimension=0, tiled=True
    ).astype(BF16)
    return (grad_input, grad_up, grad_down)


def solution(mesh):
    n, ntp = mesh.shape["fs"], mesh.shape["tp"]

    def body(inputs, cotangent, pre_act, w_up, w_down):
        rows, d = inputs.shape
        tokens, ff = pre_act.shape
        if (
            n == 8
            and ntp > 2
            and ntp % 2 == 0
            and rows <= SLAB
            and tokens % 16 == 0
            and d % 1024 == 0
            and ff % 1024 == 0
        ):
            return fused(n, ntp, inputs, cotangent, pre_act, w_up, w_down)
        return plain(inputs, cotangent, pre_act, w_up, w_down)

    return jax.shard_map(
        body,
        mesh=mesh,
        in_specs=(P("fs", "tp"), P("fs", "tp"), P(None, "fs"), P("tp", "fs"), P("fs", "tp")),
        out_specs=(P("fs", "tp"), P("tp", "fs"), P("fs", "tp")),
        check_vma=False,
    )
```

```python
import functools

import jax
import jax.numpy as jnp
from jax import lax
from jax.experimental import pallas as pl
from jax.experimental.pallas import tpu as pltpu
from jax.sharding import PartitionSpec as P

F32, BF16 = jnp.float32, jnp.bfloat16
SLAB = 8
CHUNKS = 4
AHEAD = 0
NT = (((1,), (1,)), ((), ()))
TN = (((0,), (0,)), ((), ()))
NN = (((1,), (0,)), ((), ()))


def dot(a, b, dims):
    return lax.dot_general(a, b, dims, preferred_element_type=F32)


def exchange(
    n,
    chips,
    chunks,
    cot_ref,
    in_ref,
    pre_ref,
    wu_ref,
    wd_ref,
    cot_out,
    in_out,
    act_out,
    gp_out,
    gi_out,
    own_v,
    pre_v,
    wu_v,
    wd_v,
    land,
    spread,
    own,
    p1_s,
    p1_r,
    p2_s,
    p2_r,
    rs_s,
    local,
    fs_s,
    fs_r,
    tp_s,
    gp_s,
    tp_r,
    x_r,
):
    me = lax.axis_index("fs")
    tp = lax.axis_index("tp")
    core = lax.rem(tp, 2)
    cot_v, in_v = own_v.at[0], own_v.at[1]
    cot_g, in_g, rs_r = land.at[0], land.at[1], land.at[2]
    rows = own_v.shape[1]
    width = wd_v.shape[1]
    tokens = n * rows
    half = n // 2
    side, spot = me // half, lax.rem(me, half)
    near = [half * side + lax.rem(spot + k, half) for k in range(1, half)]
    far = [half * (1 - side) + q for q in range(half)]
    partner = tp + 1 - 2 * core
    x_peer = [None] + [lax.rem(tp - core + 2 * k, 2 * chips) for k in range(1, chips)]

    barrier = pltpu.get_barrier_semaphore()
    for p in far + near:
        pl.semaphore_signal(barrier, inc=1, device_id={"fs": p})
    pl.semaphore_signal(barrier, inc=1, device_id={"tp": partner})

    @pl.when(core == 0)
    def _():
        for k in range(1, chips):
            pl.semaphore_signal(barrier, inc=1, device_id={"tp": x_peer[k]})

    def settle(ref, sem):
        pltpu.make_async_copy(ref, ref, sem).wait()

    pltpu.make_async_copy(cot_ref, cot_v, local.at[0]).start()
    pltpu.make_async_copy(in_ref, in_v, local.at[0]).start()
    for j in range(chunks):
        pltpu.make_async_copy(
            wd_ref.at[pl.ds(j * width, width)], wd_v.at[j], local.at[1]
        ).start()
    for j in range(chunks):
        pltpu.make_async_copy(
            pre_ref.at[:, pl.ds(j * width, width)], pre_v.at[j], local.at[2]
        ).start()
    for j in range(chunks):
        pltpu.make_async_copy(
            wu_ref.at[:, pl.ds(j * width, width)], wu_v.at[j], local.at[3]
        ).start()
    spread[...] = jnp.zeros_like(spread)
    settle(own_v, local.at[0])
    land[0, me] = own_v[0]
    land[1, me] = own_v[1]

    def to_fs(src, kind, p):
        return pltpu.make_async_remote_copy(
            src, land.at[kind, me], fs_s, fs_r.at[kind], device_id={"fs": p}
        )

    def from_fs(kind):
        settle(land.at[kind, pl.ds(0, n - 1)], fs_r.at[kind])

    pl.semaphore_wait(barrier, n + (1 - core) * (chips - 1))
    for p in far[::-1] + near:
        to_fs(cot_v, 0, p).start()

    def picker(shape, token_dim):
        t = lax.broadcasted_iota(jnp.int32, shape, token_dim)
        j = lax.broadcasted_iota(jnp.int32, shape, 1 - token_dim)
        q, r = j // SLAB, j % SLAB
        return ((t == q * rows + r) & (r < rows)).astype(F32).astype(BF16)

    pick = picker((tokens, n * SLAB), 0)
    place = picker((n * SLAB, tokens), 1)

    def gathered(ref):
        for s in range(n):
            spread[s * SLAB : s * SLAB + rows, :] = ref[s].astype(F32)
        return spread[...].astype(BF16)

    def between(src, dst, send_sem, recv_sem, j):
        return pltpu.make_async_remote_copy(
            src.at[j], dst.at[j], send_sem, recv_sem.at[j], device_id={"tp": partner}
        )

    def to_chip(j, k):
        return pltpu.make_async_remote_copy(
            p2_s.at[j],
            p2_r.at[k - 1, j],
            tp_s,
            x_r.at[k - 1, j],
            device_id={"tp": x_peer[k]},
        )

    def first_sum(j):
        return between(p1_s, p1_r, tp_s, tp_r, j)

    def share(j):
        return between(gp_out, gp_out, gp_s, tp_r, j)

    def lower():
        for j in range(chunks):
            p1_s[j] = dot(cot_out[...], wd_v[j], NT).astype(BF16)
            first_sum(j).start()

    def join(j):
        first_sum(j).wait_recv()
        total = own[j] + p1_r[j].astype(F32)
        own[j] = total
        p2_s[j] = total.astype(BF16)
        for k in range(1, chips):
            to_chip(j, k).start()

    def upper():
        for j in range(chunks):
            own[j] = dot(cot_out[...], wd_v[j], NT)
            join(j)

    def finish(j):
        hidden = own[j]
        for k in range(1, chips):
            to_chip(j, k).wait_recv()
            hidden = hidden + p2_r[k - 1, j].astype(F32)
        active = jnp.maximum(pre_v[j].astype(F32), 0.0)
        gp = (2.0 * active * hidden).astype(BF16)
        gp_out[j] = dot(place, gp, NN).astype(BF16)
        share(j).start()

    def obtain(j):
        share(j).wait_recv()

    def accumulate(ready, ahead):
        acc = None
        for j in range(chunks + ahead):
            if j < chunks:
                ready(j)
            if j >= ahead:
                term = dot(gp_out[j - ahead], wu_v[j - ahead], NT)
                acc = term if acc is None else acc + term
        for s in range(n):
            rs_s[s] = acc[s * SLAB : s * SLAB + rows, :].astype(BF16)
        for p in far + near:
            to_fs(rs_s.at[p], 2, p).start()

    def share_inputs():
        for p in far + near:
            to_fs(in_v, 1, p).start()

    def activate():
        settle(pre_v, local.at[2])
        for j in range(chunks):
            active = jnp.maximum(pre_v[j].astype(F32), 0.0)
            act_out[j] = (active * active).astype(BF16)

    settle(wd_v, local.at[1])
    from_fs(0)
    cot_out[...] = dot(pick, gathered(cot_g), NN).astype(BF16)

    @pl.when(core == 1)
    def _():
        lower()
        share_inputs()
        activate()
        settle(wu_v, local.at[3])
        accumulate(obtain, 0)

    @pl.when(core == 0)
    def _():
        upper()
        share_inputs()
        activate()
        settle(wu_v, local.at[3])
        accumulate(finish, AHEAD)

    from_fs(1)
    in_out[...] = gathered(in_g)

    @pl.when(core == 1)
    def _():
        settle(p1_s, tp_s)

    @pl.when(core == 0)
    def _():
        settle(p2_r, tp_s)
        settle(gp_out, gp_s)

    from_fs(2)
    total = rs_s[me].astype(F32)
    for p in near + far:
        total = total + rs_r[p].astype(F32)
    gi_out[...] = total.astype(BF16)
    settle(land.at[:, pl.ds(0, n - 1)], fs_s)


def outer(
    chunks, cot_v, in_v, act_v, gp_v, gi_v, gi_out, gu_out, gd_out, gu_v, gd_v, sem
):
    width = gp_v.shape[2]

    def put(src, dst, kind):
        pltpu.make_async_copy(src, dst, sem.at[kind]).start()

    half = width // 2
    for j in range(chunks):
        for h in range(2):
            rows = pl.ds(j * width + h * half, half)
            gd_v[rows, :] = dot(act_v[j, :, h * half : (h + 1) * half], cot_v[...], TN)
            put(gd_v.at[rows], gd_out.at[rows], 0)
    put(gi_v, gi_out, 2)
    step = in_v.shape[1] // (2 * chunks)
    for i in range(2 * chunks):
        rows = pl.ds(i * step, step)
        for j in range(chunks):
            gu_v[rows, j * width : (j + 1) * width] = dot(
                in_v[:, i * step : (i + 1) * step], gp_v[j], TN
            )
        put(gu_v.at[rows], gu_out.at[rows], 1)
    for kind, whole in enumerate((gd_v, gu_v, gi_v)):
        pltpu.make_async_copy(whole, whole, sem.at[kind]).wait()


def fused(n, ntp, inputs, cotangent, pre_act, w_up, w_down):
    rows, d = inputs.shape
    tokens, ff = pre_act.shape
    chips = ntp // 2
    chunks = CHUNKS
    width = ff // chunks
    hbm = pl.BlockSpec(memory_space=pl.ANY)
    vmem = pl.BlockSpec(memory_space=pltpu.VMEM)
    dma = pltpu.SemaphoreType.DMA
    cot, full, act, gp, gi = pl.pallas_call(
        functools.partial(exchange, n, chips, chunks),
        out_shape=(
            pltpu.VMEM((tokens, d), BF16),
            pltpu.VMEM((n * SLAB, d), BF16),
            pltpu.VMEM((chunks, tokens, width), BF16),
            pltpu.VMEM((chunks, n * SLAB, width), BF16),
            pltpu.VMEM((rows, d), BF16),
        ),
        in_specs=[hbm] * 5,
        out_specs=(vmem,) * 5,
        scratch_shapes=[
            pltpu.VMEM((2, rows, d), BF16),
            pltpu.VMEM((chunks, tokens, width), BF16),
            pltpu.VMEM((chunks, d, width), BF16),
            pltpu.VMEM((chunks, width, d), BF16),
            pltpu.VMEM((3, n, rows, d), BF16),
            pltpu.VMEM((n * SLAB, d), F32),
            pltpu.VMEM((chunks, tokens, width), F32),
            pltpu.VMEM((chunks, tokens, width), BF16),
            pltpu.VMEM((chunks, tokens, width), BF16),
            pltpu.VMEM((chunks, tokens, width), BF16),
            pltpu.VMEM((chips - 1, chunks, tokens, width), BF16),
            pltpu.VMEM((n, rows, d), BF16),
            dma((4,)),
            dma,
            dma((3,)),
            dma,
            dma,
            dma((chunks,)),
            dma((chips - 1, chunks)),
        ],
        compiler_params=pltpu.CompilerParams(collective_id=0, has_side_effects=True),
    )(cotangent, inputs, pre_act, w_up, w_down)
    return pl.pallas_call(
        functools.partial(outer, chunks),
        out_shape=(
            jax.ShapeDtypeStruct((rows, d), BF16),
            jax.ShapeDtypeStruct((d, ff), F32),
            jax.ShapeDtypeStruct((ff, d), F32),
        ),
        in_specs=[vmem] * 5,
        out_specs=(hbm,) * 3,
        scratch_shapes=[
            pltpu.VMEM((d, ff), F32),
            pltpu.VMEM((ff, d), F32),
            dma((3,)),
        ],
    )(*(pltpu.with_memory_space_constraint(x, pltpu.VMEM) for x in (cot, full, act, gp, gi)))


def plain(inputs, cotangent, pre_act, w_up, w_down):
    active = jax.nn.relu(pre_act.astype(F32))
    squared = jnp.square(active).astype(BF16)
    piece = lax.all_gather(cotangent, "fs", axis=0, tiled=True)
    grad_down = dot(squared, piece, TN)
    hidden = lax.psum(dot(piece, w_down, NT).astype(BF16), "tp").astype(F32)
    grad_pre = (2.0 * active * hidden).astype(BF16)
    grad_up = dot(lax.all_gather(inputs, "fs", axis=0, tiled=True), grad_pre, TN)
    grad_input = lax.psum_scatter(
        dot(grad_pre, w_up, NT), "fs", scatter_dimension=0, tiled=True
    ).astype(BF16)
    return (grad_input, grad_up, grad_down)


def solution(mesh):
    n, ntp = mesh.shape["fs"], mesh.shape["tp"]

    def body(inputs, cotangent, pre_act, w_up, w_down):
        rows, d = inputs.shape
        tokens, ff = pre_act.shape
        if (
            n == 8
            and ntp > 2
            and ntp % 2 == 0
            and rows <= SLAB
            and tokens % 16 == 0
            and d % 1024 == 0
            and ff % 1024 == 0
        ):
            return fused(n, ntp, inputs, cotangent, pre_act, w_up, w_down)
        return plain(inputs, cotangent, pre_act, w_up, w_down)

    return jax.shard_map(
        body,
        mesh=mesh,
        in_specs=(P("fs", "tp"), P("fs", "tp"), P(None, "fs"), P("tp", "fs"), P("fs", "tp")),
        out_specs=(P("fs", "tp"), P("tp", "fs"), P("fs", "tp")),
        check_vma=False,
    )
```

```python
import functools

import jax
import jax.numpy as jnp
from jax import lax
from jax.experimental import pallas as pl
from jax.experimental.pallas import tpu as pltpu
from jax.sharding import PartitionSpec as P

F32, BF16 = jnp.float32, jnp.bfloat16
SLAB = 8
CHUNKS = 4
AHEAD = 0
PIECES = 8
GRANT = 55 << 20
NT = (((1,), (1,)), ((), ()))
TN = (((0,), (0,)), ((), ()))
NN = (((1,), (0,)), ((), ()))


def dot(a, b, dims):
    return lax.dot_general(a, b, dims, preferred_element_type=F32)


def exchange(
    n,
    chips,
    chunks,
    cot_ref,
    in_ref,
    pre_ref,
    wu_ref,
    wd_ref,
    in_out,
    gd_out,
    gp_out,
    gi_out,
    own_v,
    pre_v,
    wu_v,
    wd_v,
    land,
    cot_out,
    packed,
    spread,
    slabs,
    own,
    p1_s,
    p1_r,
    p2_s,
    p2_r,
    rs_s,
    local,
    fs_s,
    fs_r,
    tp_s,
    gp_s,
    tp_r,
    x_r,
):
    me = lax.axis_index("fs")
    tp = lax.axis_index("tp")
    core = lax.rem(tp, 2)
    cot_v, in_v = own_v.at[0], own_v.at[1]
    cot_g, in_g, rs_r = land.at[0], land.at[1], land.at[2]
    rows = own_v.shape[1]
    width = wd_v.shape[1]
    tokens = n * rows
    half = n // 2
    side, spot = me // half, lax.rem(me, half)
    near = [half * side + lax.rem(spot + k, half) for k in range(1, half)]
    far = [half * (1 - side) + q for q in range(half)]
    partner = tp + 1 - 2 * core
    x_peer = [None] + [lax.rem(tp - core + 2 * k, 2 * chips) for k in range(1, chips)]

    barrier = pltpu.get_barrier_semaphore()
    for p in far + near:
        pl.semaphore_signal(barrier, inc=1, device_id={"fs": p})
    pl.semaphore_signal(barrier, inc=1, device_id={"tp": partner})

    @pl.when(core == 0)
    def _():
        for k in range(1, chips):
            pl.semaphore_signal(barrier, inc=1, device_id={"tp": x_peer[k]})

    def settle(ref, sem):
        pltpu.make_async_copy(ref, ref, sem).wait()

    pltpu.make_async_copy(cot_ref, cot_v, local.at[0]).start()
    pltpu.make_async_copy(in_ref, in_v, local.at[0]).start()
    for j in range(chunks):
        pltpu.make_async_copy(
            wd_ref.at[pl.ds(j * width, width)], wd_v.at[j], local.at[1]
        ).start()
    for j in range(chunks):
        pltpu.make_async_copy(
            pre_ref.at[:, pl.ds(j * width, width)], pre_v.at[j], local.at[2]
        ).start()
    for j in range(chunks):
        pltpu.make_async_copy(
            wu_ref.at[:, pl.ds(j * width, width)], wu_v.at[j], local.at[3]
        ).start()
    spread[...] = jnp.zeros_like(spread)
    slabs[...] = jnp.zeros_like(slabs)
    settle(own_v, local.at[0])
    land[0, me] = own_v[0]
    land[1, me] = own_v[1]

    def to_fs(src, kind, p):
        return pltpu.make_async_remote_copy(
            src, land.at[kind, me], fs_s, fs_r.at[kind], device_id={"fs": p}
        )

    def from_fs(kind):
        settle(land.at[kind, pl.ds(0, n - 1)], fs_r.at[kind])

    pl.semaphore_wait(barrier, n + (1 - core) * (chips - 1))
    for p in far[::-1] + near:
        to_fs(cot_v, 0, p).start()

    def gathered(ref):
        for s in range(n):
            spread[s * SLAB : s * SLAB + rows, :] = ref[s].astype(F32)
        return spread[...].astype(BF16)

    def between(src, dst, send_sem, recv_sem, j):
        return pltpu.make_async_remote_copy(
            src.at[j], dst.at[j], send_sem, recv_sem.at[j], device_id={"tp": partner}
        )

    def to_chip(j, k):
        return pltpu.make_async_remote_copy(
            p2_s.at[j],
            p2_r.at[k - 1, j],
            tp_s,
            x_r.at[k - 1, j],
            device_id={"tp": x_peer[k]},
        )

    def first_sum(j):
        return between(p1_s, p1_r, tp_s, tp_r, j)

    def share(j):
        return between(gp_out, gp_out, gp_s, tp_r, j)

    def lower():
        for j in range(chunks):
            p1_s[j] = dot(cot_out[...], wd_v[j], NT).astype(BF16)
            first_sum(j).start()

    def join(j):
        first_sum(j).wait_recv()
        total = own[j] + p1_r[j].astype(F32)
        own[j] = total
        p2_s[j] = total.astype(BF16)
        for k in range(1, chips):
            to_chip(j, k).start()

    def upper():
        for j in range(chunks):
            own[j] = dot(cot_out[...], wd_v[j], NT)
            join(j)

    def finish(j):
        hidden = own[j]
        for k in range(1, chips):
            to_chip(j, k).wait_recv()
            hidden = hidden + p2_r[k - 1, j].astype(F32)
        active = jnp.maximum(pre_v[j].astype(F32), 0.0)
        gp = 2.0 * active * hidden
        for s in range(n):
            slabs[j, s * SLAB : s * SLAB + rows, :] = gp[s * rows : (s + 1) * rows]
        gp_out[j] = slabs[j].astype(BF16)
        share(j).start()

    def obtain(j):
        share(j).wait_recv()

    def accumulate(ready, ahead):
        acc = None
        for j in range(chunks + ahead):
            if j < chunks:
                ready(j)
            if j >= ahead:
                term = dot(gp_out[j - ahead], wu_v[j - ahead], NT)
                acc = term if acc is None else acc + term
        for s in range(n):
            rs_s[s] = acc[s * SLAB : s * SLAB + rows, :].astype(BF16)
        for p in far + near:
            to_fs(rs_s.at[p], 2, p).start()

    def share_inputs():
        for p in far + near:
            to_fs(in_v, 1, p).start()

    def down():
        settle(pre_v, local.at[2])
        for j in range(chunks):
            active = jnp.maximum(pre_v[j].astype(F32), 0.0)
            act = (active * active).astype(BF16)
            for h in range(2):
                piece = slice(h * (width // 2), (h + 1) * (width // 2))
                gd_out[pl.ds(j * width + h * (width // 2), width // 2), :] = dot(
                    act[:, piece], cot_out[...], TN
                )

    settle(wd_v, local.at[1])
    from_fs(0)
    for s in range(n):
        packed[s * rows : (s + 1) * rows, :] = cot_g[s].astype(F32)
    cot_out[...] = packed[...].astype(BF16)

    @pl.when(core == 1)
    def _():
        lower()
        share_inputs()
        down()
        settle(wu_v, local.at[3])
        accumulate(obtain, 0)

    @pl.when(core == 0)
    def _():
        upper()
        share_inputs()
        down()
        settle(wu_v, local.at[3])
        accumulate(finish, AHEAD)

    from_fs(1)
    in_out[...] = gathered(in_g)

    @pl.when(core == 1)
    def _():
        settle(p1_s, tp_s)

    @pl.when(core == 0)
    def _():
        settle(p2_r, tp_s)
        settle(gp_out, gp_s)

    from_fs(2)
    total = rs_s[me].astype(F32)
    for p in near + far:
        total = total + rs_r[p].astype(F32)
    gi_out[...] = total.astype(BF16)
    settle(land.at[:, pl.ds(0, n - 1)], fs_s)


def outer(chunks, in_v, gd_v, gp_v, gi_v, gi_out, gu_out, gd_out, gu_v, sem):
    width = gp_v.shape[2]

    def put(src, dst, kind):
        pltpu.make_async_copy(src, dst, sem.at[kind]).start()

    tall = gd_v.shape[0] // PIECES
    for i in range(PIECES):
        rows = pl.ds(i * tall, tall)
        put(gd_v.at[rows], gd_out.at[rows], 0)
    put(gi_v, gi_out, 2)
    step = in_v.shape[1] // (2 * chunks)
    for i in range(2 * chunks):
        rows = pl.ds(i * step, step)
        for j in range(chunks):
            gu_v[rows, j * width : (j + 1) * width] = dot(
                in_v[:, i * step : (i + 1) * step], gp_v[j], TN
            )
        put(gu_v.at[rows], gu_out.at[rows], 1)
    for kind, whole in enumerate((gd_v, gu_v, gi_v)):
        pltpu.make_async_copy(whole, whole, sem.at[kind]).wait()


def fused(n, ntp, inputs, cotangent, pre_act, w_up, w_down):
    rows, d = inputs.shape
    tokens, ff = pre_act.shape
    chips = ntp // 2
    chunks = CHUNKS
    width = ff // chunks
    hbm = pl.BlockSpec(memory_space=pl.ANY)
    vmem = pl.BlockSpec(memory_space=pltpu.VMEM)
    dma = pltpu.SemaphoreType.DMA
    full, gd, gp, gi = pl.pallas_call(
        functools.partial(exchange, n, chips, chunks),
        out_shape=(
            pltpu.VMEM((n * SLAB, d), BF16),
            pltpu.VMEM((ff, d), F32),
            pltpu.VMEM((chunks, n * SLAB, width), BF16),
            pltpu.VMEM((rows, d), BF16),
        ),
        in_specs=[hbm] * 5,
        out_specs=(vmem,) * 4,
        scratch_shapes=[
            pltpu.VMEM((2, rows, d), BF16),
            pltpu.VMEM((chunks, tokens, width), BF16),
            pltpu.VMEM((chunks, d, width), BF16),
            pltpu.VMEM((chunks, width, d), BF16),
            pltpu.VMEM((3, n, rows, d), BF16),
            pltpu.VMEM((tokens, d), BF16),
            pltpu.VMEM((tokens, d), F32),
            pltpu.VMEM((n * SLAB, d), F32),
            pltpu.VMEM((chunks, n * SLAB, width), F32),
            pltpu.VMEM((chunks, tokens, width), F32),
            pltpu.VMEM((chunks, tokens, width), BF16),
            pltpu.VMEM((chunks, tokens, width), BF16),
            pltpu.VMEM((chunks, tokens, width), BF16),
            pltpu.VMEM((chips - 1, chunks, tokens, width), BF16),
            pltpu.VMEM((n, rows, d), BF16),
            dma((4,)),
            dma,
            dma((3,)),
            dma,
            dma,
            dma((chunks,)),
            dma((chips - 1, chunks)),
        ],
        compiler_params=pltpu.CompilerParams(
            collective_id=0, has_side_effects=True, vmem_limit_bytes=GRANT
        ),
    )(cotangent, inputs, pre_act, w_up, w_down)
    return pl.pallas_call(
        functools.partial(outer, chunks),
        out_shape=(
            jax.ShapeDtypeStruct((rows, d), BF16),
            jax.ShapeDtypeStruct((d, ff), F32),
            jax.ShapeDtypeStruct((ff, d), F32),
        ),
        in_specs=[vmem] * 4,
        out_specs=(hbm,) * 3,
        scratch_shapes=[
            pltpu.VMEM((d, ff), F32),
            dma((3,)),
        ],
        compiler_params=pltpu.CompilerParams(vmem_limit_bytes=GRANT),
    )(*(pltpu.with_memory_space_constraint(x, pltpu.VMEM) for x in (full, gd, gp, gi)))


def plain(inputs, cotangent, pre_act, w_up, w_down):
    active = jax.nn.relu(pre_act.astype(F32))
    squared = jnp.square(active).astype(BF16)
    piece = lax.all_gather(cotangent, "fs", axis=0, tiled=True)
    grad_down = dot(squared, piece, TN)
    hidden = lax.psum(dot(piece, w_down, NT).astype(BF16), "tp").astype(F32)
    grad_pre = (2.0 * active * hidden).astype(BF16)
    grad_up = dot(lax.all_gather(inputs, "fs", axis=0, tiled=True), grad_pre, TN)
    grad_input = lax.psum_scatter(
        dot(grad_pre, w_up, NT), "fs", scatter_dimension=0, tiled=True
    ).astype(BF16)
    return (grad_input, grad_up, grad_down)


def solution(mesh):
    n, ntp = mesh.shape["fs"], mesh.shape["tp"]

    def body(inputs, cotangent, pre_act, w_up, w_down):
        rows, d = inputs.shape
        tokens, ff = pre_act.shape
        if (
            n == 8
            and ntp > 2
            and ntp % 2 == 0
            and rows <= SLAB
            and tokens % 16 == 0
            and d % 1024 == 0
            and ff % 1024 == 0
        ):
            return fused(n, ntp, inputs, cotangent, pre_act, w_up, w_down)
        return plain(inputs, cotangent, pre_act, w_up, w_down)

    return jax.shard_map(
        body,
        mesh=mesh,
        in_specs=(P("fs", "tp"), P("fs", "tp"), P(None, "fs"), P("tp", "fs"), P("fs", "tp")),
        out_specs=(P("fs", "tp"), P("tp", "fs"), P("fs", "tp")),
        check_vma=False,
    )
```

```python
import functools

import jax
import jax.numpy as jnp
from jax import lax
from jax.experimental import pallas as pl
from jax.experimental.pallas import tpu as pltpu
from jax.sharding import PartitionSpec as P

F32, BF16 = jnp.float32, jnp.bfloat16
SLAB = 8
CHUNKS = 4
AHEAD = 0
PIECES = 8
GRANT = 55 << 20
NT = (((1,), (1,)), ((), ()))
TN = (((0,), (0,)), ((), ()))
NN = (((1,), (0,)), ((), ()))


def dot(a, b, dims):
    return lax.dot_general(a, b, dims, preferred_element_type=F32)


def exchange(
    n,
    chips,
    chunks,
    cot_ref,
    in_ref,
    pre_ref,
    wu_ref,
    wd_ref,
    in_out,
    gd_out,
    gp_out,
    gi_out,
    own_v,
    pre_v,
    wu_v,
    wd_v,
    land,
    cot_out,
    packed,
    spread,
    slabs,
    own,
    p1_s,
    p1_r,
    p2_s,
    p2_r,
    rs_s,
    local,
    fs_s,
    fs_r,
    tp_s,
    gp_s,
    tp_r,
    x_r,
):
    me = lax.axis_index("fs")
    tp = lax.axis_index("tp")
    core = lax.rem(tp, 2)
    cot_v, in_v = own_v.at[0], own_v.at[1]
    cot_g, in_g, rs_r = land.at[0], land.at[1], land.at[2]
    rows = own_v.shape[1]
    width = wd_v.shape[1]
    tokens = n * rows
    half = n // 2
    side, spot = me // half, lax.rem(me, half)
    near = [half * side + lax.rem(spot + k, half) for k in range(1, half)]
    far = [half * (1 - side) + q for q in range(half)]
    partner = tp + 1 - 2 * core
    x_peer = [None] + [lax.rem(tp - core + 2 * k, 2 * chips) for k in range(1, chips)]

    barrier = pltpu.get_barrier_semaphore()
    for p in far + near:
        pl.semaphore_signal(barrier, inc=1, device_id={"fs": p})
    pl.semaphore_signal(barrier, inc=1, device_id={"tp": partner})

    @pl.when(core == 0)
    def _():
        for k in range(1, chips):
            pl.semaphore_signal(barrier, inc=1, device_id={"tp": x_peer[k]})

    def settle(ref, sem):
        pltpu.make_async_copy(ref, ref, sem).wait()

    pltpu.make_async_copy(cot_ref, cot_v, local.at[0]).start()
    pltpu.make_async_copy(in_ref, in_v, local.at[0]).start()
    for j in range(chunks):
        pltpu.make_async_copy(
            wd_ref.at[pl.ds(j * width, width)], wd_v.at[j], local.at[1]
        ).start()
    for j in range(chunks):
        pltpu.make_async_copy(
            pre_ref.at[:, pl.ds(j * width, width)], pre_v.at[j], local.at[2]
        ).start()
    for j in range(chunks):
        pltpu.make_async_copy(
            wu_ref.at[:, pl.ds(j * width, width)], wu_v.at[j], local.at[3]
        ).start()
    spread[...] = jnp.zeros_like(spread)
    slabs[...] = jnp.zeros_like(slabs)
    settle(own_v, local.at[0])
    land[0, me] = own_v[0]
    land[1, me] = own_v[1]

    def to_fs(src, kind, p):
        return pltpu.make_async_remote_copy(
            src, land.at[kind, me], fs_s, fs_r.at[kind], device_id={"fs": p}
        )

    def from_fs(kind):
        settle(land.at[kind, pl.ds(0, n - 1)], fs_r.at[kind])

    pl.semaphore_wait(barrier, n + (1 - core) * (chips - 1))
    for p in far[::-1] + near:
        to_fs(cot_v, 0, p).start()

    def gathered(ref):
        for s in range(n):
            spread[s * SLAB : s * SLAB + rows, :] = ref[s].astype(F32)
        return spread[...].astype(BF16)

    def between(src, dst, send_sem, recv_sem, j):
        return pltpu.make_async_remote_copy(
            src.at[j], dst.at[j], send_sem, recv_sem.at[j], device_id={"tp": partner}
        )

    def to_chip(j, k):
        return pltpu.make_async_remote_copy(
            p2_s.at[j],
            p2_r.at[k - 1, j],
            tp_s,
            x_r.at[k - 1, j],
            device_id={"tp": x_peer[k]},
        )

    def first_sum(j):
        return between(p1_s, p1_r, tp_s, tp_r, j)

    def share(j):
        return between(gp_out, gp_out, gp_s, tp_r, j)

    def lower():
        for j in range(chunks):
            p1_s[j] = dot(cot_out[...], wd_v[j], NT).astype(BF16)
            first_sum(j).start()

    def join(j):
        first_sum(j).wait_recv()
        total = own[j] + p1_r[j].astype(F32)
        own[j] = total
        p2_s[j] = total.astype(BF16)
        for k in range(1, chips):
            to_chip(j, k).start()

    def upper():
        for j in range(chunks):
            own[j] = dot(cot_out[...], wd_v[j], NT)
            join(j)

    def finish(j):
        hidden = own[j]
        for k in range(1, chips):
            to_chip(j, k).wait_recv()
            hidden = hidden + p2_r[k - 1, j].astype(F32)
        active = jnp.maximum(pre_v[j].astype(F32), 0.0)
        gp = 2.0 * active * hidden
        for s in range(n):
            slabs[j, s * SLAB : s * SLAB + rows, :] = gp[s * rows : (s + 1) * rows]
        gp_out[j] = slabs[j].astype(BF16)
        share(j).start()

    def obtain(j):
        share(j).wait_recv()

    def accumulate(ready, ahead):
        acc = None
        for j in range(chunks + ahead):
            if j < chunks:
                ready(j)
            if j >= ahead:
                term = dot(gp_out[j - ahead], wu_v[j - ahead], NT)
                acc = term if acc is None else acc + term
        for s in range(n):
            rs_s[s] = acc[s * SLAB : s * SLAB + rows, :].astype(BF16)
        for p in [far[0], near[0], far[1], near[1], far[2], near[2], far[3]]:
            to_fs(rs_s.at[p], 2, p).start()

    def share_inputs():
        for p in far + near:
            to_fs(in_v, 1, p).start()

    def down():
        settle(pre_v, local.at[2])
        for j in range(chunks):
            active = jnp.maximum(pre_v[j].astype(F32), 0.0)
            act = (active * active).astype(BF16)
            for h in range(2):
                piece = slice(h * (width // 2), (h + 1) * (width // 2))
                gd_out[pl.ds(j * width + h * (width // 2), width // 2), :] = dot(
                    act[:, piece], cot_out[...], TN
                )

    settle(wd_v, local.at[1])
    from_fs(0)
    for s in range(n):
        packed[s * rows : (s + 1) * rows, :] = cot_g[s].astype(F32)
    cot_out[...] = packed[...].astype(BF16)

    @pl.when(core == 1)
    def _():
        lower()
        share_inputs()
        down()
        settle(wu_v, local.at[3])
        accumulate(obtain, 0)

    @pl.when(core == 0)
    def _():
        upper()
        share_inputs()
        down()
        settle(wu_v, local.at[3])
        accumulate(finish, AHEAD)

    from_fs(1)
    in_out[...] = gathered(in_g)

    @pl.when(core == 1)
    def _():
        settle(p1_s, tp_s)

    @pl.when(core == 0)
    def _():
        settle(p2_r, tp_s)
        settle(gp_out, gp_s)

    from_fs(2)
    total = rs_s[me].astype(F32)
    for p in near + far:
        total = total + rs_r[p].astype(F32)
    gi_out[...] = total.astype(BF16)
    settle(land.at[:, pl.ds(0, n - 1)], fs_s)


def outer(chunks, in_v, gd_v, gp_v, gi_v, gi_out, gu_out, gd_out, gu_v, sem):
    width = gp_v.shape[2]

    def put(src, dst, kind):
        pltpu.make_async_copy(src, dst, sem.at[kind]).start()

    tall = gd_v.shape[0] // PIECES
    for i in range(PIECES):
        rows = pl.ds(i * tall, tall)
        put(gd_v.at[rows], gd_out.at[rows], 0)
    put(gi_v, gi_out, 2)
    step = in_v.shape[1] // (2 * chunks)
    for i in range(2 * chunks):
        rows = pl.ds(i * step, step)
        for j in range(chunks):
            gu_v[rows, j * width : (j + 1) * width] = dot(
                in_v[:, i * step : (i + 1) * step], gp_v[j], TN
            )
        put(gu_v.at[rows], gu_out.at[rows], 1)
    for kind, whole in enumerate((gd_v, gu_v, gi_v)):
        pltpu.make_async_copy(whole, whole, sem.at[kind]).wait()


def fused(n, ntp, inputs, cotangent, pre_act, w_up, w_down):
    rows, d = inputs.shape
    tokens, ff = pre_act.shape
    chips = ntp // 2
    chunks = CHUNKS
    width = ff // chunks
    hbm = pl.BlockSpec(memory_space=pl.ANY)
    vmem = pl.BlockSpec(memory_space=pltpu.VMEM)
    dma = pltpu.SemaphoreType.DMA
    full, gd, gp, gi = pl.pallas_call(
        functools.partial(exchange, n, chips, chunks),
        out_shape=(
            pltpu.VMEM((n * SLAB, d), BF16),
            pltpu.VMEM((ff, d), F32),
            pltpu.VMEM((chunks, n * SLAB, width), BF16),
            pltpu.VMEM((rows, d), BF16),
        ),
        in_specs=[hbm] * 5,
        out_specs=(vmem,) * 4,
        scratch_shapes=[
            pltpu.VMEM((2, rows, d), BF16),
            pltpu.VMEM((chunks, tokens, width), BF16),
            pltpu.VMEM((chunks, d, width), BF16),
            pltpu.VMEM((chunks, width, d), BF16),
            pltpu.VMEM((3, n, rows, d), BF16),
            pltpu.VMEM((tokens, d), BF16),
            pltpu.VMEM((tokens, d), F32),
            pltpu.VMEM((n * SLAB, d), F32),
            pltpu.VMEM((chunks, n * SLAB, width), F32),
            pltpu.VMEM((chunks, tokens, width), F32),
            pltpu.VMEM((chunks, tokens, width), BF16),
            pltpu.VMEM((chunks, tokens, width), BF16),
            pltpu.VMEM((chunks, tokens, width), BF16),
            pltpu.VMEM((chips - 1, chunks, tokens, width), BF16),
            pltpu.VMEM((n, rows, d), BF16),
            dma((4,)),
            dma,
            dma((3,)),
            dma,
            dma,
            dma((chunks,)),
            dma((chips - 1, chunks)),
        ],
        compiler_params=pltpu.CompilerParams(
            collective_id=0, has_side_effects=True, vmem_limit_bytes=GRANT
        ),
    )(cotangent, inputs, pre_act, w_up, w_down)
    return pl.pallas_call(
        functools.partial(outer, chunks),
        out_shape=(
            jax.ShapeDtypeStruct((rows, d), BF16),
            jax.ShapeDtypeStruct((d, ff), F32),
            jax.ShapeDtypeStruct((ff, d), F32),
        ),
        in_specs=[vmem] * 4,
        out_specs=(hbm,) * 3,
        scratch_shapes=[
            pltpu.VMEM((d, ff), F32),
            dma((3,)),
        ],
        compiler_params=pltpu.CompilerParams(vmem_limit_bytes=GRANT),
    )(*(pltpu.with_memory_space_constraint(x, pltpu.VMEM) for x in (full, gd, gp, gi)))


def plain(inputs, cotangent, pre_act, w_up, w_down):
    active = jax.nn.relu(pre_act.astype(F32))
    squared = jnp.square(active).astype(BF16)
    piece = lax.all_gather(cotangent, "fs", axis=0, tiled=True)
    grad_down = dot(squared, piece, TN)
    hidden = lax.psum(dot(piece, w_down, NT).astype(BF16), "tp").astype(F32)
    grad_pre = (2.0 * active * hidden).astype(BF16)
    grad_up = dot(lax.all_gather(inputs, "fs", axis=0, tiled=True), grad_pre, TN)
    grad_input = lax.psum_scatter(
        dot(grad_pre, w_up, NT), "fs", scatter_dimension=0, tiled=True
    ).astype(BF16)
    return (grad_input, grad_up, grad_down)


def solution(mesh):
    n, ntp = mesh.shape["fs"], mesh.shape["tp"]

    def body(inputs, cotangent, pre_act, w_up, w_down):
        rows, d = inputs.shape
        tokens, ff = pre_act.shape
        if (
            n == 8
            and ntp > 2
            and ntp % 2 == 0
            and rows <= SLAB
            and tokens % 16 == 0
            and d % 1024 == 0
            and ff % 1024 == 0
        ):
            return fused(n, ntp, inputs, cotangent, pre_act, w_up, w_down)
        return plain(inputs, cotangent, pre_act, w_up, w_down)

    return jax.shard_map(
        body,
        mesh=mesh,
        in_specs=(P("fs", "tp"), P("fs", "tp"), P(None, "fs"), P("tp", "fs"), P("fs", "tp")),
        out_specs=(P("fs", "tp"), P("tp", "fs"), P("fs", "tp")),
        check_vma=False,
    )
```
